32 devices in a mesh: sp: 8 (over z, x), tp: 4 (over y, core).
Axes of the slice: x: 2, y: 2, z: 4, core: 2. Of those that a mesh axis runs over, the one named last changes fastest.
Arguments:
- activations: bfloat16 [6144, 2048], P('sp'), may hold values from -6 to 6
- norm_gain: bfloat16 [2048], replicated, may hold values from 0.099609375 to 1.8984375
- w_conv_outer: bfloat16 [2048, 1024], P(None, 'tp'), may hold values from -0.125 to 0.125
- w_conv_inner: bfloat16 [2048, 1024], P(None, 'tp'), may hold values from -0.125 to 0.125
- w_conv_value: bfloat16 [2048, 1024], P(None, 'tp'), may hold values from -0.125 to 0.125
- conv_taps: bfloat16 [3, 1024], P(None, 'tp'), may hold values from -3 to 3
- w_query: bfloat16 [2048, 1024], P(None, 'tp'), may hold values from -0.125 to 0.125
- w_key: bfloat16 [2048, 1024], P(None, 'tp'), may hold values from -0.125 to 0.125
- w_value: bfloat16 [2048, 1024], P(None, 'tp'), may hold values from -0.125 to 0.125
- w_gate: bfloat16 [2048, 1024], P(None, 'tp'), may hold values from -0.125 to 0.125
- log_decay: float32 [8, 6144], P('tp', 'sp'), may hold values from -2.5 to 0
- w_out_conv: bfloat16 [1024, 2048], P('tp'), may hold values from -0.125 to 0.125
- w_out_ret: bfloat16 [1024, 2048], P('tp'), may hold values from -0.125 to 0.125
Outputs:
- mixed: bfloat16 [6144, 2048], P(('sp', 'tp'))
The draws below stay inside these ranges and needn't reach their ends.
All inputs are finite; a program needn't handle non-finite values.
Results may differ from the reference program's by a relative error of at most 0.02.
Values may be sent and summed in bfloat16 or wider, within the bound.
A program may use at most 128 MiB of HBM per device.

```python
import jax
import jax.numpy as jnp
from jax import lax

D = 2048
CONV_CH = 1024
HEAD = 128
RETENTION_HEADS = 8
CONV_W = 3
BLK = 128
TOK_DEV = 768
RET_CH = 1024
TOKEN_COUNT = 6144
N_TP = 4


def draw_log_decay(key, part):
    random_keys_split = jax.random.split(jax.random.fold_in(key, 7), 6)
    ranking = jax.random.permutation(random_keys_split[0], RETENTION_HEADS)
    quick_heads = ranking < RETENTION_HEADS // 2
    slow_rate = 0.5 / TOKEN_COUNT
    quick_rate = jax.random.uniform(random_keys_split[1], (RETENTION_HEADS,), jnp.float32, 1.0 / 80.0, 1.0 / 30.0)
    base_rate = jnp.where(quick_heads, quick_rate, slow_rate)
    span_count = TOKEN_COUNT // TOK_DEV
    span_factor = jnp.exp(jax.random.uniform(random_keys_split[2], (RETENTION_HEADS, span_count, 1), jnp.float32, jnp.log(0.4), jnp.log(2.5)))
    jitter = jax.random.uniform(random_keys_split[3], (RETENTION_HEADS, span_count, TOK_DEV), jnp.float32, 0.5, 1.5)
    decay_factor = (base_rate[:, None, None] * span_factor * jitter).reshape(RETENTION_HEADS, TOKEN_COUNT)
    spike_position = jax.random.randint(random_keys_split[4], (RETENTION_HEADS, 3), 0, TOKEN_COUNT)
    spike_penalty = jax.random.uniform(random_keys_split[5], (RETENTION_HEADS, 3), jnp.float32, 0.2, 0.5)
    match_lookup = (jnp.arange(TOKEN_COUNT, dtype=jnp.int32)[None, None, :] == spike_position[:, :, None]).astype(jnp.float32)
    spike_total = jnp.sum(match_lookup * jnp.log(1.0 - spike_penalty)[:, :, None], axis=1)
    return -decay_factor + spike_total


def block_levels(key, dims, cuts, least, high):
    def one(position, blocks):
        steps = jax.random.uniform(jax.random.fold_in(jax.random.fold_in(key, 6), position), (blocks,), jnp.float32, least / len(cuts), high / len(cuts))
        return jnp.repeat(jnp.exp(steps), dims[position] // blocks).reshape((-1,) + (1,) * (len(dims) - position - 1))

    loudness = one(*cuts[0])
    for cut in cuts[1:]:
        loudness = loudness * one(*cut)
    return loudness


def normal_values(stream_key, extent, spread, bound, pieces=(), held_as=jnp.bfloat16):
    entries = jax.random.normal(stream_key, extent, jnp.float32) * spread
    if len(pieces) > 0:
        entries = block_levels(stream_key, extent, pieces, -0.22, 0.18) * entries
    return jnp.clip(entries, min=-bound, max=bound).astype(held_as)


def setup_inputs(seed: int = 0) -> dict:
    arg_keys = jax.random.split(jax.random.key(seed), 14)
    activations = normal_values(arg_keys[0], (TOKEN_COUNT, D), 1.0, 6.0, ((0, 8),))
    norm_gain = jnp.clip(1.0 + 0.18 * jax.random.normal(arg_keys[1], (D,), jnp.float32), 0.099609375, 1.8984375).astype(jnp.bfloat16)
    w_conv_outer = normal_values(arg_keys[2], (D, CONV_CH), D ** -0.5, 0.125, ((1, 4),))
    w_conv_inner = normal_values(arg_keys[3], (D, CONV_CH), D ** -0.5, 0.125, ((1, 4),))
    w_conv_value = normal_values(arg_keys[4], (D, CONV_CH), D ** -0.5, 0.125, ((1, 4),))
    conv_taps = normal_values(arg_keys[5], (CONV_W, CONV_CH), 0.577, 3.0, ((1, 4),))
    w_query = normal_values(arg_keys[6], (D, RET_CH), D ** -0.5, 0.125, ((1, 4),))
    w_key = normal_values(arg_keys[7], (D, RET_CH), D ** -0.5, 0.125, ((1, 4),))
    w_value = normal_values(arg_keys[8], (D, RET_CH), D ** -0.5, 0.125, ((1, 4),))
    w_gate = normal_values(arg_keys[9], (D, RET_CH), D ** -0.5, 0.125, ((1, 4),))
    log_decay = draw_log_decay(jax.random.fold_in(arg_keys[13], 71), 0)
    w_out_conv = normal_values(arg_keys[11], (CONV_CH, D), (CONV_CH + RET_CH) ** -0.5, 0.125, ((0, 4),))
    w_out_ret = normal_values(arg_keys[12], (RET_CH, D), (CONV_CH + RET_CH) ** -0.5, 0.125, ((0, 4),))
    return dict(activations=activations, norm_gain=norm_gain, w_conv_outer=w_conv_outer, w_conv_inner=w_conv_inner, w_conv_value=w_conv_value, conv_taps=conv_taps, w_query=w_query, w_key=w_key, w_value=w_value, w_gate=w_gate, log_decay=log_decay, w_out_conv=w_out_conv, w_out_ret=w_out_ret)


EPS = 1e-06

def rotate_heads(block, positions):
    half_dim = block.shape[-1] // 2
    inverse = 10000.0 ** (-jnp.arange(half_dim, dtype=jnp.float32) / half_dim)
    angles = positions[:, None] * inverse[None, :]
    cosine = jnp.cos(angles)[:, None, :]
    sine_part = jnp.sin(angles)[:, None, :]
    widened = block.astype(jnp.float32)
    first = widened[..., :half_dim]
    second = widened[..., half_dim:]
    turned = jnp.concatenate([first * cosine - second * sine_part, second * cosine + first * sine_part], axis=-1)
    return turned.astype(jnp.bfloat16)

def project(normed, weight):
    result = jnp.dot(normed, weight, preferred_element_type=jnp.float32).astype(jnp.bfloat16)
    return lax.optimization_barrier(result)

def reference(activations, norm_gain, w_conv_outer, w_conv_inner, w_conv_value, conv_taps, w_query, w_key, w_value, w_gate, log_decay, w_out_conv, w_out_ret):
    total_rows = activations.shape[0]
    widened = activations.astype(jnp.float32)
    normed = (widened * lax.rsqrt(lax.optimization_barrier(jnp.mean(widened * widened, axis=-1, keepdims=True)) + EPS) * norm_gain.astype(jnp.float32)).astype(jnp.bfloat16)
    normed = lax.optimization_barrier(normed)
    conv_outer = project(normed, w_conv_outer)
    conv_inner = project(normed, w_conv_inner)
    conv_value = project(normed, w_conv_value)
    product = (conv_inner.astype(jnp.float32) * conv_value.astype(jnp.float32)).astype(jnp.bfloat16)
    product = lax.optimization_barrier(product)
    extended = jnp.concatenate([jnp.zeros((CONV_W - 1, product.shape[1]), jnp.bfloat16), product], axis=0).astype(jnp.float32)
    taps = conv_taps.astype(jnp.float32)
    filtered = taps[0][None, :] * extended[0:total_rows]
    for tap_index in range(1, CONV_W):
        filtered = filtered + taps[tap_index][None, :] * extended[tap_index:tap_index + total_rows]
    conv_out = (conv_outer.astype(jnp.float32) * filtered).astype(jnp.bfloat16)
    conv_out = lax.optimization_barrier(conv_out)
    positions = jnp.arange(total_rows, dtype=jnp.int32).astype(jnp.float32)
    query = rotate_heads(project(normed, w_query).reshape(total_rows, RETENTION_HEADS, HEAD), positions)
    key_rot = rotate_heads(project(normed, w_key).reshape(total_rows, RETENTION_HEADS, HEAD), positions)
    query = lax.optimization_barrier(query)
    key_rot = lax.optimization_barrier(key_rot)
    values = project(normed, w_value).reshape(total_rows, RETENTION_HEADS, HEAD)
    gate_pre = project(normed, w_gate).reshape(total_rows, RETENTION_HEADS, HEAD)
    blocks = total_rows // BLK
    levels = jnp.cumsum(log_decay.reshape(RETENTION_HEADS, blocks, BLK), axis=2).transpose(1, 0, 2)
    causal = jnp.arange(BLK)[:, None] >= jnp.arange(BLK)[None, :]

    def block_step(state, inputs):
        q_blk, k_blk, v_blk, lev = inputs
        scores = jnp.einsum('ihd,jhd->hij', q_blk.astype(jnp.float32), k_blk.astype(jnp.float32))
        diff = lev[:, :, None] - lev[:, None, :]
        decay_tab = jnp.exp(jnp.where(causal[None], diff, -1e+30))
        weights = (scores * decay_tab).astype(jnp.bfloat16)
        weights = lax.optimization_barrier(weights)
        inner_part = jnp.einsum('hij,jhd->ihd', weights.astype(jnp.float32), v_blk.astype(jnp.float32))
        total = lev[:, BLK - 1]
        query_dec = q_blk.astype(jnp.float32) * jnp.exp(lev).T[:, :, None]
        cross = jnp.einsum('ihd,hde->ihe', query_dec, state, precision=lax.Precision.HIGHEST)
        key_dec = k_blk.astype(jnp.float32) * jnp.exp(total[:, None] - lev).T[:, :, None]
        contrib = jnp.einsum('jhd,jhe->hde', key_dec, v_blk.astype(jnp.float32), precision=lax.Precision.HIGHEST)
        state = state * jnp.exp(total)[:, None, None] + contrib
        return (state, inner_part + cross)
    start_state = jnp.zeros((RETENTION_HEADS, HEAD, HEAD), jnp.float32)
    inputs = (query.reshape(blocks, BLK, RETENTION_HEADS, HEAD), key_rot.reshape(blocks, BLK, RETENTION_HEADS, HEAD), values.reshape(blocks, BLK, RETENTION_HEADS, HEAD), levels)
    final_state, retained = lax.scan(block_step, start_state, inputs)
    retained = retained.reshape(total_rows, RETENTION_HEADS, HEAD)
    mean_sq = lax.optimization_barrier(jnp.mean(retained * retained, axis=-1, keepdims=True))
    ret_out = (retained * lax.rsqrt(mean_sq + EPS) * jax.nn.silu(gate_pre.astype(jnp.float32))).astype(jnp.bfloat16)
    ret_out = lax.optimization_barrier(ret_out.reshape(total_rows, RETENTION_HEADS * HEAD))
    conv_group = CONV_CH // N_TP
    head_group = RETENTION_HEADS * HEAD // N_TP
    mixed_sum = jnp.zeros((total_rows, D), jnp.float32)
    for group_index in range(N_TP):
        conv_part = conv_out[:, group_index * conv_group:(group_index + 1) * conv_group]
        ret_part = ret_out[:, group_index * head_group:(group_index + 1) * head_group]
        partial_sum = jnp.dot(conv_part, w_out_conv[group_index * conv_group:(group_index + 1) * conv_group], preferred_element_type=jnp.float32)
        partial_sum = partial_sum + jnp.dot(ret_part, w_out_ret[group_index * head_group:(group_index + 1) * head_group], preferred_element_type=jnp.float32)
        rounded = lax.optimization_barrier(partial_sum.astype(jnp.bfloat16))
        mixed_sum = mixed_sum + rounded.astype(jnp.float32)
    return mixed_sum.astype(jnp.bfloat16)
```

```python
import functools

import jax
import jax.numpy as jnp
import numpy as np
from jax import lax
from jax.experimental import pallas as pl
from jax.experimental.pallas import tpu as pltpu
from jax.sharding import PartitionSpec as P

HEAD = 128
CONV_W = 3
BLK = 128
EPS = 1e-06
MESH = pl.DeviceIdType.MESH
F32 = jnp.float32
BF16 = jnp.bfloat16
HI = lax.Precision.HIGHEST


def windows_of(size):
    widths, width = [], 1
    while width < size:
        widths.append(width)
        width *= 3
    return widths


def rotary_tables(total_blocks):
    half = HEAD // 2
    inverse = 10000.0 ** (-np.arange(half, dtype=np.float64) / half)
    sign = np.concatenate([-np.ones(half), np.ones(half)])

    def table(positions):
        angles = positions[:, None] * np.concatenate([inverse, inverse])[None, :]
        return np.cos(angles).astype(np.float32), (np.sin(angles) * sign).astype(np.float32)

    return table(np.arange(BLK, dtype=np.float64)) + table(
        np.arange(total_blocks, dtype=np.float64) * BLK
    )


def kernel(
    n_sp,
    chunks,
    acts_hbm,
    gain_ref,
    wco_hbm,
    wci_hbm,
    wcv_hbm,
    taps_ref,
    wq_hbm,
    wk_hbm,
    wv_hbm,
    wg_hbm,
    decay_ref,
    woc_hbm,
    wor_hbm,
    cos_in_ref,
    sin_in_ref,
    cos_off_ref,
    sin_off_ref,
    out_ref,
    x_ref,
    w_ref,
    wo_ref,
    k_ref,
    v_ref,
    q_ref,
    g_ref,
    co_ref,
    ext_ref,
    inner_ref,
    mix_ref,
    st_ref,
    cs_ref,
    sn_ref,
    ld_ref,
    run_ref,
    es_ref,
    el_ref,
    send_s,
    send_l,
    recv_s,
    recv_l,
    send_a,
    recv_a,
    own_ref,
    send_b,
    recv_b,
    x_sem,
    w_sem,
    scan_send_sem,
    scan_recv_sem,
    rim_sem,
    a_sem,
    b_sem,
):
    sp = lax.axis_index("sp")
    tp = lax.axis_index("tp")
    rows, width = x_ref.shape
    heads = decay_ref.shape[0]
    ch = co_ref.shape[1]
    rc = heads * HEAD
    blocks = rows // BLK
    tiles = blocks
    proj = 256 if rows % 256 == 0 else BLK
    widths = windows_of(n_sp)
    distances = [d for w in widths for d in (w, 2 * w) if d < n_sp]
    sibling, across = tp ^ 1, tp ^ 2

    x_copies = [
        pltpu.make_async_copy(
            acts_hbm.at[pl.ds(i * BLK, BLK)], x_ref.at[pl.ds(i * BLK, BLK)], x_sem.at[i]
        )
        for i in range(tiles)
    ]
    bounds, w_copies = {}, {}
    start = 0
    for index, (name, ref) in enumerate(
        (
            ("k", wk_hbm),
            ("v", wv_hbm),
            ("q", wq_hbm),
            ("g", wg_hbm),
            ("ci", wci_hbm),
            ("cv", wcv_hbm),
            ("co", wco_hbm),
        )
    ):
        size = ref.shape[1]
        bounds[name] = (start, start + size)
        w_copies[name] = pltpu.make_async_copy(
            ref, w_ref.at[:, pl.ds(start, size)], w_sem.at[index]
        )
        start += size
    w_copies["oc"] = pltpu.make_async_copy(woc_hbm, wo_ref.at[pl.ds(0, ch)], w_sem.at[7])
    w_copies["or"] = pltpu.make_async_copy(wor_hbm, wo_ref.at[pl.ds(ch, rc)], w_sem.at[8])
    for copy in x_copies:
        copy.start()
    for name in ("k", "v", "q", "g", "ci", "cv", "co", "oc", "or"):
        w_copies[name].start()

    barrier = pltpu.get_barrier_semaphore()
    expected = jnp.int32(2)
    for peer in (sibling, across):
        pl.semaphore_signal(barrier, inc=1, device_id=(sp, peer), device_id_type=MESH)
    for d in distances:
        @pl.when(sp + d < n_sp)
        def _(d=d):
            pl.semaphore_signal(barrier, inc=1, device_id=(sp + d, tp), device_id_type=MESH)

        @pl.when(sp >= d)
        def _(d=d):
            pl.semaphore_signal(barrier, inc=1, device_id=(sp - d, tp), device_id_type=MESH)

        expected = (
            expected
            + jnp.where(sp + d < n_sp, jnp.int32(1), jnp.int32(0))
            + jnp.where(sp >= d, jnp.int32(1), jnp.int32(0))
        )

    for b in range(blocks):
        c_off = cos_off_ref[pl.ds(sp * blocks + b, 1), :]
        s_off = sin_off_ref[pl.ds(sp * blocks + b, 1), :]
        c_in, s_in = cos_in_ref[...], sin_in_ref[...]
        cs_ref[pl.ds(b * BLK, BLK), :] = c_off * c_in - s_off * s_in
        sn_ref[pl.ds(b * BLK, BLK), :] = s_off * c_in + c_off * s_in

    ld_ref[...] = jnp.zeros_like(ld_ref)
    for h in range(heads):
        for b in range(blocks):
            j = h * blocks + b
            ld_ref[j : j + 1, :] = decay_ref[h : h + 1, b * BLK : (b + 1) * BLK]
    ld = ld_ref[...]
    row_i = lax.broadcasted_iota(jnp.int32, (BLK, BLK), 0)
    col_i = lax.broadcasted_iota(jnp.int32, (BLK, BLK), 1)
    causal = row_i >= col_i
    upper = jnp.where(row_i <= col_i, 1.0, 0.0).astype(F32)
    lower = jnp.where(row_i >= col_i, 1.0, 0.0).astype(F32)
    after = jnp.where(row_i < col_i, 1.0, 0.0).astype(F32)
    ones = jnp.ones((BLK, BLK), F32)
    nt = (((1,), (1,)), ((), ()))
    level_row = jnp.dot(ld, upper, precision=HI, preferred_element_type=F32)
    total_row = jnp.dot(ld, ones, precision=HI, preferred_element_type=F32)
    level_col = lax.dot_general(lower, ld, nt, precision=HI, preferred_element_type=F32)
    rest_col = lax.dot_general(after, ld, nt, precision=HI, preferred_element_type=F32)
    key_scale = jnp.exp(rest_col)
    query_scale = jnp.exp(level_col)

    def norm_tile(i, carry):
        at = pl.ds(pl.multiple_of(i * BLK, BLK), BLK)
        pltpu.make_async_copy(acts_hbm.at[at], x_ref.at[at], x_sem.at[i]).wait()
        x = x_ref[at, :].astype(F32)
        mean_sq = jnp.mean(x * x, axis=-1, keepdims=True)
        x_ref[at, :] = (x * lax.rsqrt(mean_sq + EPS) * gain_ref[...].astype(F32)).astype(BF16)
        return carry

    lax.fori_loop(0, tiles, norm_tile, 0)

    def project(at, first, last):
        lo, hi = bounds[first][0], bounds[last][1]
        return jnp.dot(x_ref[at, :], w_ref[:, lo:hi], preferred_element_type=F32).astype(BF16)

    def rotate(part, at):
        cosine, sine = cs_ref[at, :], sn_ref[at, :]
        turned = []
        for h in range(heads):
            wide = part[:, h * HEAD : (h + 1) * HEAD].astype(F32)
            turned.append((wide * cosine + pltpu.roll(wide, HEAD // 2, 1) * sine).astype(BF16))
        return turned

    def tile_at(i):
        return pl.ds(pl.multiple_of(i * proj, proj), proj)

    w_copies["k"].wait()
    w_copies["v"].wait()

    def kv_tile(i, carry):
        at = tile_at(i)
        both = project(at, "k", "v")
        v_ref[at, :] = both[:, rc:]
        for h, turned in enumerate(rotate(both[:, :rc], at)):
            k_ref[at, h * HEAD : (h + 1) * HEAD] = turned
        return carry

    lax.fori_loop(0, rows // proj, kv_tile, 0)

    device_total = []
    starts = []
    for h in range(heads):
        running = jnp.zeros((HEAD, HEAD), F32)
        total = jnp.zeros((1, HEAD), F32)
        cols = slice(h * HEAD, (h + 1) * HEAD)
        for b in range(blocks):
            j = h * blocks + b
            st_ref[j] = running
            starts.append(total)
            at = slice(b * BLK, (b + 1) * BLK)
            k_dec = (k_ref[at, cols].astype(F32) * key_scale[:, j : j + 1]).astype(BF16)
            contrib = lax.dot_general(
                k_dec, v_ref[at, cols], (((0,), (0,)), ((), ())), preferred_element_type=F32
            )
            running = running * jnp.exp(total_row[j : j + 1, :]) + contrib
            total = total + total_row[j : j + 1, :]
        run_ref[cols, :] = running
        device_total.append(total)

    pl.semaphore_wait(barrier, expected)

    es_ref[...] = jnp.zeros_like(es_ref)
    el_ref[...] = jnp.zeros_like(el_ref)
    send_l[...] = jnp.zeros_like(send_l)

    def scan_copies(r, j, d):
        to = (sp + d, tp)
        return (
            pltpu.make_async_remote_copy(
                src_ref=send_s.at[r],
                dst_ref=recv_s.at[r, j],
                send_sem=scan_send_sem.at[r, j, 0],
                recv_sem=scan_recv_sem.at[r, j, 0],
                device_id=to,
                device_id_type=MESH,
            ),
            pltpu.make_async_remote_copy(
                src_ref=send_l.at[r],
                dst_ref=recv_l.at[r, j],
                send_sem=scan_send_sem.at[r, j, 1],
                recv_sem=scan_recv_sem.at[r, j, 1],
                device_id=to,
                device_id_type=MESH,
            ),
        )

    def scan_send(r):
        for h in range(heads):
            cols = slice(h * HEAD, (h + 1) * HEAD)
            state = run_ref[cols, :]
            if r > 0:
                state = state + jnp.exp(device_total[h]) * es_ref[cols, :]
            send_s[r, cols, :] = state.astype(BF16)
            send_l[r, h : h + 1, :] = device_total[h] + el_ref[h : h + 1, :]
        for j in range(2):
            d = (j + 1) * widths[r]
            if d < n_sp:
                @pl.when(sp + d < n_sp)
                def _(j=j, d=d):
                    for copy in scan_copies(r, j, d):
                        copy.start()

    def scan_receive(r):
        for j in range(2):
            d = (j + 1) * widths[r]
            if d < n_sp:
                @pl.when(sp >= d)
                def _(j=j, d=d):
                    for copy in scan_copies(r, j, d):
                        copy.wait_recv()
                    for h in range(heads):
                        cols = slice(h * HEAD, (h + 1) * HEAD)
                        es_ref[cols, :] += jnp.exp(el_ref[h : h + 1, :]) * recv_s[
                            r, j, cols, :
                        ].astype(F32)
                    el_ref[...] += recv_l[r, j]

    scan_send(0)

    w_copies["q"].wait()
    w_copies["g"].wait()

    def qg_tile(i, carry):
        at = tile_at(i)
        both = project(at, "q", "g")
        g_ref[at, :] = both[:, rc:]
        for h, turned in enumerate(rotate(both[:, :rc], at)):
            q_ref[at, h * HEAD : (h + 1) * HEAD] = turned
        return carry

    lax.fori_loop(0, rows // proj, qg_tile, 0)

    for r in range(1, len(widths)):
        scan_receive(r - 1)
        scan_send(r)

    for name in ("ci", "cv", "co"):
        w_copies[name].wait()

    def conv_tile(i, carry):
        at = tile_at(i)
        three = project(at, "ci", "co")
        product = (three[:, :ch].astype(F32) * three[:, ch : 2 * ch].astype(F32)).astype(BF16)
        ext_ref[pl.ds(pl.multiple_of(i * proj + 8, 8), proj), :] = product.astype(F32)
        co_ref[at, :] = three[:, 2 * ch :]
        return carry

    lax.fori_loop(0, rows // proj, conv_tile, 0)

    rim = pltpu.make_async_remote_copy(
        src_ref=ext_ref.at[pl.ds(rows, 8)],
        dst_ref=ext_ref.at[pl.ds(0, 8)],
        send_sem=rim_sem.at[0],
        recv_sem=rim_sem.at[1],
        device_id=(sp + 1, tp),
        device_id_type=MESH,
    )

    @pl.when(sp == 0)
    def _():
        ext_ref[pl.ds(0, 8), :] = jnp.zeros((8, ch), F32)

    @pl.when(sp + 1 < n_sp)
    def _():
        rim.start()

    for h in range(heads):
        cols = slice(h * HEAD, (h + 1) * HEAD)
        for b in range(blocks):
            j = h * blocks + b
            at = slice(b * BLK, (b + 1) * BLK)
            scores = lax.dot_general(q_ref[at, cols], k_ref[at, cols], nt, preferred_element_type=F32)
            diff = level_col[:, j : j + 1] - level_row[j : j + 1, :]
            weights = (scores * jnp.exp(jnp.where(causal, diff, -1e30))).astype(BF16)
            inner_ref[at, cols] = jnp.dot(weights, v_ref[at, cols], preferred_element_type=F32)

    @pl.when(sp >= 1)
    def _():
        rim.wait_recv()

    taps = taps_ref[...].astype(F32)
    for b in range(blocks):
        at = slice(b * BLK, (b + 1) * BLK)
        base = b * BLK + 8 - (CONV_W - 1)
        filtered = taps[0:1, :] * ext_ref[base : base + BLK, :]
        for t in range(1, CONV_W):
            filtered = filtered + taps[t : t + 1, :] * ext_ref[base + t : base + t + BLK, :]
        mix_ref[at, 0:ch] = (co_ref[at, :].astype(F32) * filtered).astype(BF16)

    scan_receive(len(widths) - 1)

    for b in range(blocks):
        at = slice(b * BLK, (b + 1) * BLK)
        for h in range(heads):
            cols = slice(h * HEAD, (h + 1) * HEAD)
            j = h * blocks + b
            state = (st_ref[j] + jnp.exp(starts[j]) * es_ref[cols, :]).astype(BF16)
            q_dec = (q_ref[at, cols].astype(F32) * query_scale[:, j : j + 1]).astype(BF16)
            retained = inner_ref[at, cols] + jnp.dot(q_dec, state, preferred_element_type=F32)
            mean_sq = jnp.mean(retained * retained, axis=-1, keepdims=True)
            gate = g_ref[at, cols].astype(F32)
            gate = gate / (1.0 + jnp.exp(-gate))
            mix_ref[at, ch + h * HEAD : ch + (h + 1) * HEAD] = (
                retained * lax.rsqrt(mean_sq + EPS) * gate
            ).astype(BF16)

    w_copies["oc"].wait()
    w_copies["or"].wait()
    part = out_ref.shape[0]
    wide = width // chunks

    def partial(block, c):
        at = pl.ds(pl.multiple_of(block * part, 16), part)
        return jnp.dot(
            mix_ref[at, :], wo_ref[:, c * wide : (c + 1) * wide], preferred_element_type=F32
        )

    def to_sibling(p, c):
        return pltpu.make_async_remote_copy(
            src_ref=send_a.at[p, c],
            dst_ref=recv_a.at[p, c],
            send_sem=a_sem.at[0, p, c],
            recv_sem=a_sem.at[1, p, c],
            device_id=(sp, sibling),
            device_id_type=MESH,
        )

    def to_across(c):
        return pltpu.make_async_remote_copy(
            src_ref=send_b.at[c],
            dst_ref=recv_b.at[c],
            send_sem=b_sem.at[0, c],
            recv_sem=b_sem.at[1, c],
            device_id=(sp, across),
            device_id_type=MESH,
        )

    def send_sibling(p, c):
        send_a[p, c] = partial(tp ^ (3 if p == 0 else 1), c).astype(BF16)
        to_sibling(p, c).start()

    def send_across(c):
        own = partial(across, c)
        to_sibling(0, c).wait_recv()
        send_b[c] = (own + recv_a[0, c].astype(F32)).astype(BF16)
        to_across(c).start()

    send_sibling(0, 0)
    for c in range(chunks):
        if c + 1 < chunks:
            send_sibling(0, c + 1)
        send_across(c)
    for c in range(chunks):
        send_sibling(1, c)
    for c in range(chunks):
        own_ref[c] = partial(tp, c)
    for c in range(chunks):
        to_sibling(1, c).wait_recv()
        own_ref[c] += recv_a[1, c].astype(F32)
    for c in range(chunks):
        to_across(c).wait_recv()
        out_ref[:, c * wide : (c + 1) * wide] = (own_ref[c] + recv_b[c].astype(F32)).astype(BF16)

    for r in range(len(widths)):
        for j in range(2):
            d = (j + 1) * widths[r]
            if d < n_sp:
                @pl.when(sp + d < n_sp)
                def _(r=r, j=j, d=d):
                    for copy in scan_copies(r, j, d):
                        copy.wait_send()

    @pl.when(sp + 1 < n_sp)
    def _():
        rim.wait_send()

    for c in range(chunks):
        to_sibling(0, c).wait_send()
        to_sibling(1, c).wait_send()
        to_across(c).wait_send()


def local(
    n_sp,
    n_tp,
    activations,
    norm_gain,
    w_conv_outer,
    w_conv_inner,
    w_conv_value,
    conv_taps,
    w_query,
    w_key,
    w_value,
    w_gate,
    log_decay,
    w_out_conv,
    w_out_ret,
):
    rows, width = activations.shape
    heads = log_decay.shape[0]
    blocks = rows // BLK
    ch = w_conv_outer.shape[1]
    rc = heads * HEAD
    part = rows // n_tp
    chunks = 4
    wide = width // chunks
    rounds = len(windows_of(n_sp))
    pad = -(-heads * blocks // 8) * 8
    tables = [jnp.asarray(t) for t in rotary_tables(n_sp * blocks)]
    vmem = pl.BlockSpec(memory_space=pltpu.VMEM)
    hbm = pl.BlockSpec(memory_space=pl.ANY)
    dma = pltpu.SemaphoreType.DMA
    return pl.pallas_call(
        functools.partial(kernel, n_sp, chunks),
        out_shape=jax.ShapeDtypeStruct((part, width), BF16),
        in_specs=[hbm, vmem, hbm, hbm, hbm, vmem, hbm, hbm, hbm, hbm, vmem, hbm, hbm] + [vmem] * 4,
        out_specs=vmem,
        scratch_shapes=[
            pltpu.VMEM((rows, width), BF16),
            pltpu.VMEM((width, 3 * ch + 4 * rc), BF16),
            pltpu.VMEM((ch + rc, width), BF16),
            pltpu.VMEM((rows, rc), BF16),
            pltpu.VMEM((rows, rc), BF16),
            pltpu.VMEM((rows, rc), BF16),
            pltpu.VMEM((rows, rc), BF16),
            pltpu.VMEM((rows, ch), BF16),
            pltpu.VMEM((rows + 8, ch), F32),
            pltpu.VMEM((rows, rc), F32),
            pltpu.VMEM((rows, ch + rc), BF16),
            pltpu.VMEM((heads * blocks, HEAD, HEAD), F32),
            pltpu.VMEM((rows, HEAD), F32),
            pltpu.VMEM((rows, HEAD), F32),
            pltpu.VMEM((pad, BLK), F32),
            pltpu.VMEM((rc, HEAD), F32),
            pltpu.VMEM((rc, HEAD), F32),
            pltpu.VMEM((8, HEAD), F32),
            pltpu.VMEM((rounds, rc, HEAD), BF16),
            pltpu.VMEM((rounds, 8, HEAD), F32),
            pltpu.VMEM((rounds, 2, rc, HEAD), BF16),
            pltpu.VMEM((rounds, 2, 8, HEAD), F32),
            pltpu.VMEM((2, chunks, part, wide), BF16),
            pltpu.VMEM((2, chunks, part, wide), BF16),
            pltpu.VMEM((chunks, part, wide), F32),
            pltpu.VMEM((chunks, part, wide), BF16),
            pltpu.VMEM((chunks, part, wide), BF16),
            dma((blocks,)),
            dma((9,)),
            dma((rounds, 2, 2)),
            dma((rounds, 2, 2)),
            dma((2,)),
            dma((2, 2, chunks)),
            dma((2, chunks)),
        ],
        compiler_params=pltpu.CompilerParams(
            collective_id=0, has_side_effects=True, vmem_limit_bytes=60 * 1024 * 1024
        ),
    )(
        activations,
        norm_gain.reshape(1, width),
        w_conv_outer,
        w_conv_inner,
        w_conv_value,
        conv_taps,
        w_query,
        w_key,
        w_value,
        w_gate,
        log_decay,
        w_out_conv,
        w_out_ret,
        *tables,
    )


def solution(mesh):
    return jax.shard_map(
        functools.partial(local, mesh.shape["sp"], mesh.shape["tp"]),
        mesh=mesh,
        in_specs=(
            P("sp", None),
            P(),
            P(None, "tp"),
            P(None, "tp"),
            P(None, "tp"),
            P(None, "tp"),
            P(None, "tp"),
            P(None, "tp"),
            P(None, "tp"),
            P(None, "tp"),
            P("tp", "sp"),
            P("tp", None),
            P("tp", None),
        ),
        out_specs=P(("sp", "tp"), None),
        check_vma=False,
    )
```

```python
import functools

import jax
import jax.numpy as jnp
import numpy as np
from jax import lax
from jax.experimental import pallas as pl
from jax.experimental.pallas import tpu as pltpu
from jax.sharding import PartitionSpec as P

HEAD = 128
CONV_W = 3
BLK = 128
EPS = 1e-06
MESH = pl.DeviceIdType.MESH
F32 = jnp.float32
BF16 = jnp.bfloat16
HI = lax.Precision.HIGHEST


def windows_of(size):
    widths, width = [], 1
    while width < size:
        widths.append(width)
        width *= 3
    return widths


def rotary_tables(total_blocks):
    half = HEAD // 2
    inverse = 10000.0 ** (-np.arange(half, dtype=np.float64) / half)
    sign = np.concatenate([-np.ones(half), np.ones(half)])

    def table(positions):
        angles = positions[:, None] * np.concatenate([inverse, inverse])[None, :]
        return np.cos(angles).astype(np.float32), (np.sin(angles) * sign).astype(np.float32)

    return table(np.arange(BLK, dtype=np.float64)) + table(
        np.arange(total_blocks, dtype=np.float64) * BLK
    )


def kernel(
    n_sp,
    chunks,
    acts_hbm,
    gain_hbm,
    wco_hbm,
    wci_hbm,
    wcv_hbm,
    taps_hbm,
    wq_hbm,
    wk_hbm,
    wv_hbm,
    wg_hbm,
    decay_hbm,
    woc_hbm,
    wor_hbm,
    cos_in_hbm,
    sin_in_hbm,
    cos_off_hbm,
    sin_off_hbm,
    own_out,
    recv_b,
    gain_ref,
    taps_ref,
    decay_ref,
    cos_in_ref,
    sin_in_ref,
    cos_off_ref,
    sin_off_ref,
    x_ref,
    w_ref,
    wo_ref,
    k_ref,
    v_ref,
    q_ref,
    g_ref,
    co_ref,
    ext_ref,
    inner_ref,
    mix_ref,
    st_ref,
    cs_ref,
    sn_ref,
    ld_ref,
    run_ref,
    es_ref,
    el_ref,
    send_s,
    send_l,
    recv_s,
    recv_l,
    send_a,
    recv_a,
    own_ref,
    send_b,
    small_sem,
    out_sem,
    x_sem,
    w_sem,
    scan_send_sem,
    scan_recv_sem,
    rim_sem,
    a_sem,
    b_sem,
):
    sp = lax.axis_index("sp")
    tp = lax.axis_index("tp")
    rows, width = x_ref.shape
    heads = decay_ref.shape[0]
    ch = co_ref.shape[1]
    rc = heads * HEAD
    blocks = rows // BLK
    proj = 256 if rows % 256 == 0 else BLK
    tiles = rows // proj
    widths = windows_of(n_sp)
    distances = [d for w in widths for d in (w, 2 * w) if d < n_sp]
    sibling, across = tp ^ 1, tp ^ 2

    x_copies = [
        pltpu.make_async_copy(
            acts_hbm.at[pl.ds(i * proj, proj)], x_ref.at[pl.ds(i * proj, proj)], x_sem.at[i]
        )
        for i in range(tiles)
    ]
    bounds, w_copies = {}, {}
    start = 0
    for index, (name, ref) in enumerate(
        (
            ("k", wk_hbm),
            ("v", wv_hbm),
            ("q", wq_hbm),
            ("g", wg_hbm),
            ("ci", wci_hbm),
            ("cv", wcv_hbm),
            ("co", wco_hbm),
        )
    ):
        size = ref.shape[1]
        bounds[name] = (start, start + size)
        w_copies[name] = pltpu.make_async_copy(
            ref, w_ref.at[:, pl.ds(start, size)], w_sem.at[index]
        )
        start += size
    w_copies["oc"] = pltpu.make_async_copy(woc_hbm, wo_ref.at[pl.ds(0, ch)], w_sem.at[7])
    w_copies["or"] = pltpu.make_async_copy(wor_hbm, wo_ref.at[pl.ds(ch, rc)], w_sem.at[8])
    small = [
        pltpu.make_async_copy(src, dst, small_sem.at[index])
        for index, (src, dst) in enumerate(
            (
                (decay_hbm, decay_ref),
                (gain_hbm, gain_ref),
                (cos_off_hbm, cos_off_ref),
                (sin_off_hbm, sin_off_ref),
                (cos_in_hbm, cos_in_ref),
                (sin_in_hbm, sin_in_ref),
                (taps_hbm, taps_ref),
            )
        )
    ]
    for copy in small[:2] + x_copies[:1]:
        copy.start()
    w_copies["k"].start()
    w_copies["v"].start()
    for copy in x_copies[1:] + small[2:]:
        copy.start()
    for name in ("q", "g", "ci", "cv", "co", "oc", "or"):
        w_copies[name].start()

    barrier = pltpu.get_barrier_semaphore()
    expected = jnp.int32(2)
    for peer in (sibling, across):
        pl.semaphore_signal(barrier, inc=1, device_id=(sp, peer), device_id_type=MESH)
    for d in distances:
        @pl.when(sp + d < n_sp)
        def _(d=d):
            pl.semaphore_signal(barrier, inc=1, device_id=(sp + d, tp), device_id_type=MESH)

        @pl.when(sp >= d)
        def _(d=d):
            pl.semaphore_signal(barrier, inc=1, device_id=(sp - d, tp), device_id_type=MESH)

        expected = (
            expected
            + jnp.where(sp + d < n_sp, jnp.int32(1), jnp.int32(0))
            + jnp.where(sp >= d, jnp.int32(1), jnp.int32(0))
        )

    small[0].wait()
    ld_ref[...] = jnp.zeros_like(ld_ref)
    for h in range(heads):
        for b in range(blocks):
            j = h * blocks + b
            ld_ref[j : j + 1, :] = decay_ref[h : h + 1, b * BLK : (b + 1) * BLK]
    ld = ld_ref[...]
    row_i = lax.broadcasted_iota(jnp.int32, (BLK, BLK), 0)
    col_i = lax.broadcasted_iota(jnp.int32, (BLK, BLK), 1)
    causal = row_i >= col_i
    upper = jnp.where(row_i <= col_i, 1.0, 0.0).astype(F32)
    lower = jnp.where(row_i >= col_i, 1.0, 0.0).astype(F32)
    after = jnp.where(row_i < col_i, 1.0, 0.0).astype(F32)
    ones = jnp.ones((BLK, BLK), F32)
    nt = (((1,), (1,)), ((), ()))
    level_row = jnp.dot(ld, upper, precision=HI, preferred_element_type=F32)
    total_row = jnp.dot(ld, ones, precision=HI, preferred_element_type=F32)
    level_col = lax.dot_general(lower, ld, nt, precision=HI, preferred_element_type=F32)
    rest_col = lax.dot_general(after, ld, nt, precision=HI, preferred_element_type=F32)
    key_scale = jnp.exp(rest_col)
    query_scale = jnp.exp(level_col)

    small[1].wait()
    gain = gain_ref[...].astype(F32)[None, :]

    def norm_tile(i):
        at = slice(i * proj, (i + 1) * proj)
        x = x_ref[at, :].astype(F32)
        mean_sq = jnp.mean(x * x, axis=-1, keepdims=True)
        x_ref[at, :] = (x * lax.rsqrt(mean_sq + EPS) * gain).astype(BF16)

    x_copies[0].wait()
    norm_tile(0)

    for copy in small[2:]:
        copy.wait()
    for b in range(blocks):
        c_off = cos_off_ref[pl.ds(sp * blocks + b, 1), :]
        s_off = sin_off_ref[pl.ds(sp * blocks + b, 1), :]
        c_in, s_in = cos_in_ref[...], sin_in_ref[...]
        cs_ref[pl.ds(b * BLK, BLK), :] = c_off * c_in - s_off * s_in
        sn_ref[pl.ds(b * BLK, BLK), :] = s_off * c_in + c_off * s_in

    def project(at, first, last):
        lo, hi = bounds[first][0], bounds[last][1]
        return jnp.dot(x_ref[at, :], w_ref[:, lo:hi], preferred_element_type=F32).astype(BF16)

    def rotate(part, at):
        cosine, sine = cs_ref[at, :], sn_ref[at, :]
        turned = []
        for h in range(heads):
            wide = part[:, h * HEAD : (h + 1) * HEAD].astype(F32)
            turned.append((wide * cosine + pltpu.roll(wide, HEAD // 2, 1) * sine).astype(BF16))
        return turned

    def tile_at(i):
        return pl.ds(pl.multiple_of(i * proj, proj), proj)

    w_copies["k"].wait()
    w_copies["v"].wait()
    for copy in x_copies[1:]:
        copy.wait()
    for i in range(tiles):
        at = slice(i * proj, (i + 1) * proj)
        both = project(at, "k", "v")
        if i + 1 < tiles:
            norm_tile(i + 1)
        v_ref[at, :] = both[:, rc:]
        for h, turned in enumerate(rotate(both[:, :rc], at)):
            k_ref[at, h * HEAD : (h + 1) * HEAD] = turned

    device_total = []
    starts = []
    for h in range(heads):
        running = jnp.zeros((HEAD, HEAD), F32)
        total = jnp.zeros((1, HEAD), F32)
        cols = slice(h * HEAD, (h + 1) * HEAD)
        for b in range(blocks):
            j = h * blocks + b
            st_ref[j] = running
            starts.append(total)
            at = slice(b * BLK, (b + 1) * BLK)
            k_dec = (k_ref[at, cols].astype(F32) * key_scale[:, j : j + 1]).astype(BF16)
            contrib = lax.dot_general(
                k_dec, v_ref[at, cols], (((0,), (0,)), ((), ())), preferred_element_type=F32
            )
            running = running * jnp.exp(total_row[j : j + 1, :]) + contrib
            total = total + total_row[j : j + 1, :]
        run_ref[cols, :] = running
        device_total.append(total)

    pl.semaphore_wait(barrier, expected)

    es_ref[...] = jnp.zeros_like(es_ref)
    el_ref[...] = jnp.zeros_like(el_ref)
    send_l[...] = jnp.zeros_like(send_l)

    def scan_copies(r, j, d):
        to = (sp + d, tp)
        return (
            pltpu.make_async_remote_copy(
                src_ref=send_s.at[r],
                dst_ref=recv_s.at[r, j],
                send_sem=scan_send_sem.at[r, j, 0],
                recv_sem=scan_recv_sem.at[r, j, 0],
                device_id=to,
                device_id_type=MESH,
            ),
            pltpu.make_async_remote_copy(
                src_ref=send_l.at[r],
                dst_ref=recv_l.at[r, j],
                send_sem=scan_send_sem.at[r, j, 1],
                recv_sem=scan_recv_sem.at[r, j, 1],
                device_id=to,
                device_id_type=MESH,
            ),
        )

    def scan_send(r):
        for h in range(heads):
            cols = slice(h * HEAD, (h + 1) * HEAD)
            state = run_ref[cols, :]
            if r > 0:
                state = state + jnp.exp(device_total[h]) * es_ref[cols, :]
            send_s[r, cols, :] = state.astype(BF16)
            send_l[r, h : h + 1, :] = device_total[h] + el_ref[h : h + 1, :]
        for j in range(2):
            d = (j + 1) * widths[r]
            if d < n_sp:
                @pl.when(sp + d < n_sp)
                def _(j=j, d=d):
                    for copy in scan_copies(r, j, d):
                        copy.start()

    def scan_receive(r):
        for j in range(2):
            d = (j + 1) * widths[r]
            if d < n_sp:
                @pl.when(sp >= d)
                def _(j=j, d=d):
                    for copy in scan_copies(r, j, d):
                        copy.wait_recv()
                    for h in range(heads):
                        cols = slice(h * HEAD, (h + 1) * HEAD)
                        es_ref[cols, :] += jnp.exp(el_ref[h : h + 1, :]) * recv_s[
                            r, j, cols, :
                        ].astype(F32)
                    el_ref[...] += recv_l[r, j]

    scan_send(0)

    w_copies["q"].wait()
    w_copies["g"].wait()

    def qg_tile(i, carry):
        at = tile_at(i)
        both = project(at, "q", "g")
        g_ref[at, :] = both[:, rc:]
        for h, turned in enumerate(rotate(both[:, :rc], at)):
            q_ref[at, h * HEAD : (h + 1) * HEAD] = turned
        return carry

    lax.fori_loop(0, rows // proj, qg_tile, 0)

    for r in range(1, len(widths)):
        scan_receive(r - 1)
        scan_send(r)

    for name in ("ci", "cv", "co"):
        w_copies[name].wait()

    def conv_tile(i, carry):
        at = tile_at(i)
        three = project(at, "ci", "co")
        product = (three[:, :ch].astype(F32) * three[:, ch : 2 * ch].astype(F32)).astype(BF16)
        ext_ref[pl.ds(pl.multiple_of(i * proj + 8, 8), proj), :] = product.astype(F32)
        co_ref[at, :] = three[:, 2 * ch :]
        return carry

    lax.fori_loop(0, rows // proj, conv_tile, 0)

    rim = pltpu.make_async_remote_copy(
        src_ref=ext_ref.at[pl.ds(rows, 8)],
        dst_ref=ext_ref.at[pl.ds(0, 8)],
        send_sem=rim_sem.at[0],
        recv_sem=rim_sem.at[1],
        device_id=(sp + 1, tp),
        device_id_type=MESH,
    )

    @pl.when(sp == 0)
    def _():
        ext_ref[pl.ds(0, 8), :] = jnp.zeros((8, ch), F32)

    @pl.when(sp + 1 < n_sp)
    def _():
        rim.start()

    for h in range(heads):
        cols = slice(h * HEAD, (h + 1) * HEAD)
        for b in range(blocks):
            j = h * blocks + b
            at = slice(b * BLK, (b + 1) * BLK)
            scores = lax.dot_general(q_ref[at, cols], k_ref[at, cols], nt, preferred_element_type=F32)
            diff = level_col[:, j : j + 1] - level_row[j : j + 1, :]
            weights = (scores * jnp.exp(jnp.where(causal, diff, -1e30))).astype(BF16)
            inner_ref[at, cols] = jnp.dot(weights, v_ref[at, cols], preferred_element_type=F32)

    @pl.when(sp >= 1)
    def _():
        rim.wait_recv()

    taps = taps_ref[...].astype(F32)
    for b in range(blocks):
        at = slice(b * BLK, (b + 1) * BLK)
        base = b * BLK + 8 - (CONV_W - 1)
        filtered = taps[0:1, :] * ext_ref[base : base + BLK, :]
        for t in range(1, CONV_W):
            filtered = filtered + taps[t : t + 1, :] * ext_ref[base + t : base + t + BLK, :]
        mix_ref[at, 0:ch] = (co_ref[at, :].astype(F32) * filtered).astype(BF16)

    scan_receive(len(widths) - 1)

    for b in range(blocks):
        at = slice(b * BLK, (b + 1) * BLK)
        for h in range(heads):
            cols = slice(h * HEAD, (h + 1) * HEAD)
            j = h * blocks + b
            state = (st_ref[j] + jnp.exp(starts[j]) * es_ref[cols, :]).astype(BF16)
            q_dec = (q_ref[at, cols].astype(F32) * query_scale[:, j : j + 1]).astype(BF16)
            retained = inner_ref[at, cols] + jnp.dot(q_dec, state, preferred_element_type=F32)
            mean_sq = jnp.mean(retained * retained, axis=-1, keepdims=True)
            gate = g_ref[at, cols].astype(F32)
            gate = gate / (1.0 + jnp.exp(-gate))
            mix_ref[at, ch + h * HEAD : ch + (h + 1) * HEAD] = (
                retained * lax.rsqrt(mean_sq + EPS) * gate
            ).astype(BF16)

    w_copies["oc"].wait()
    w_copies["or"].wait()
    part = own_out.shape[0]
    wide = width // chunks

    def partial(block, c):
        at = pl.ds(pl.multiple_of(block * part, 16), part)
        return jnp.dot(
            mix_ref[at, :], wo_ref[:, c * wide : (c + 1) * wide], preferred_element_type=F32
        )

    def to_sibling(p, c):
        return pltpu.make_async_remote_copy(
            src_ref=send_a.at[p, c],
            dst_ref=recv_a.at[p, c],
            send_sem=a_sem.at[0, p, c],
            recv_sem=a_sem.at[1, p, c],
            device_id=(sp, sibling),
            device_id_type=MESH,
        )

    def to_across(c):
        return pltpu.make_async_remote_copy(
            src_ref=send_b.at[c],
            dst_ref=recv_b.at[:, pl.ds(c * wide, wide)],
            send_sem=b_sem.at[0, c],
            recv_sem=b_sem.at[1, c],
            device_id=(sp, across),
            device_id_type=MESH,
        )

    def send_sibling(p, c):
        send_a[p, c] = partial(tp ^ (3 if p == 0 else 1), c).astype(BF16)
        to_sibling(p, c).start()

    def send_across(c):
        own = partial(across, c)
        to_sibling(0, c).wait_recv()
        send_b[c] = (own + recv_a[0, c].astype(F32)).astype(BF16)
        to_across(c).start()

    send_sibling(0, 0)
    for c in range(chunks):
        if c + 1 < chunks:
            send_sibling(0, c + 1)
        send_across(c)
    for c in range(chunks):
        send_sibling(1, c)
    outs = [
        pltpu.make_async_copy(
            own_ref.at[c], own_out.at[:, pl.ds(c * wide, wide)], out_sem.at[c]
        )
        for c in range(chunks)
    ]
    for c in range(chunks):
        own = partial(tp, c)
        to_sibling(1, c).wait_recv()
        own_ref[c] = (own + recv_a[1, c].astype(F32)).astype(BF16)
        outs[c].start()

    for r in range(len(widths)):
        for j in range(2):
            d = (j + 1) * widths[r]
            if d < n_sp:
                @pl.when(sp + d < n_sp)
                def _(r=r, j=j, d=d):
                    for copy in scan_copies(r, j, d):
                        copy.wait_send()

    @pl.when(sp + 1 < n_sp)
    def _():
        rim.wait_send()

    for c in range(chunks):
        to_sibling(0, c).wait_send()
        to_sibling(1, c).wait_send()
        outs[c].wait()
        to_across(c).wait()


def local(
    n_sp,
    n_tp,
    activations,
    norm_gain,
    w_conv_outer,
    w_conv_inner,
    w_conv_value,
    conv_taps,
    w_query,
    w_key,
    w_value,
    w_gate,
    log_decay,
    w_out_conv,
    w_out_ret,
):
    rows, width = activations.shape
    heads = log_decay.shape[0]
    blocks = rows // BLK
    ch = w_conv_outer.shape[1]
    rc = heads * HEAD
    part = rows // n_tp
    chunks = 4
    wide = width // chunks
    rounds = len(windows_of(n_sp))
    pad = -(-heads * blocks // 8) * 8
    tables = [jnp.asarray(t) for t in rotary_tables(n_sp * blocks)]
    hbm = pl.BlockSpec(memory_space=pl.ANY)
    dma = pltpu.SemaphoreType.DMA
    own, received = pl.pallas_call(
        functools.partial(kernel, n_sp, chunks),
        out_shape=[jax.ShapeDtypeStruct((part, width), BF16)] * 2,
        in_specs=[hbm] * 17,
        out_specs=[hbm] * 2,
        scratch_shapes=[
            pltpu.VMEM(norm_gain.shape, BF16),
            pltpu.VMEM(conv_taps.shape, BF16),
            pltpu.VMEM(log_decay.shape, F32),
            pltpu.VMEM((BLK, HEAD), F32),
            pltpu.VMEM((BLK, HEAD), F32),
            pltpu.VMEM((n_sp * blocks, HEAD), F32),
            pltpu.VMEM((n_sp * blocks, HEAD), F32),
            pltpu.VMEM((rows, width), BF16),
            pltpu.VMEM((width, 3 * ch + 4 * rc), BF16),
            pltpu.VMEM((ch + rc, width), BF16),
            pltpu.VMEM((rows, rc), BF16),
            pltpu.VMEM((rows, rc), BF16),
            pltpu.VMEM((rows, rc), BF16),
            pltpu.VMEM((rows, rc), BF16),
            pltpu.VMEM((rows, ch), BF16),
            pltpu.VMEM((rows + 8, ch), F32),
            pltpu.VMEM((rows, rc), F32),
            pltpu.VMEM((rows, ch + rc), BF16),
            pltpu.VMEM((heads * blocks, HEAD, HEAD), F32),
            pltpu.VMEM((rows, HEAD), F32),
            pltpu.VMEM((rows, HEAD), F32),
            pltpu.VMEM((pad, BLK), F32),
            pltpu.VMEM((rc, HEAD), F32),
            pltpu.VMEM((rc, HEAD), F32),
            pltpu.VMEM((8, HEAD), F32),
            pltpu.VMEM((rounds, rc, HEAD), BF16),
            pltpu.VMEM((rounds, 8, HEAD), F32),
            pltpu.VMEM((rounds, 2, rc, HEAD), BF16),
            pltpu.VMEM((rounds, 2, 8, HEAD), F32),
            pltpu.VMEM((2, chunks, part, wide), BF16),
            pltpu.VMEM((2, chunks, part, wide), BF16),
            pltpu.VMEM((chunks, part, wide), BF16),
            pltpu.VMEM((chunks, part, wide), BF16),
            dma((7,)),
            dma((chunks,)),
            dma((blocks,)),
            dma((9,)),
            dma((rounds, 2, 2)),
            dma((rounds, 2, 2)),
            dma((2,)),
            dma((2, 2, chunks)),
            dma((2, chunks)),
        ],
        compiler_params=pltpu.CompilerParams(
            collective_id=0, has_side_effects=True, vmem_limit_bytes=60 * 1024 * 1024
        ),
    )(
        activations,
        norm_gain,
        w_conv_outer,
        w_conv_inner,
        w_conv_value,
        conv_taps,
        w_query,
        w_key,
        w_value,
        w_gate,
        log_decay,
        w_out_conv,
        w_out_ret,
        *tables,
    )
    return (own.astype(F32) + received.astype(F32)).astype(BF16)


def solution(mesh):
    return jax.shard_map(
        functools.partial(local, mesh.shape["sp"], mesh.shape["tp"]),
        mesh=mesh,
        in_specs=(
            P("sp", None),
            P(),
            P(None, "tp"),
            P(None, "tp"),
            P(None, "tp"),
            P(None, "tp"),
            P(None, "tp"),
            P(None, "tp"),
            P(None, "tp"),
            P(None, "tp"),
            P("tp", "sp"),
            P("tp", None),
            P("tp", None),
        ),
        out_specs=P(("sp", "tp"), None),
        check_vma=False,
    )
```

```python
import functools

import jax
import jax.numpy as jnp
import numpy as np
from jax import lax
from jax.experimental import pallas as pl
from jax.experimental.pallas import tpu as pltpu
from jax.sharding import PartitionSpec as P

HEAD = 128
CONV_W = 3
BLK = 128
EPS = 1e-06
MESH = pl.DeviceIdType.MESH
F32 = jnp.float32
BF16 = jnp.bfloat16
HI = lax.Precision.HIGHEST


def windows_of(size):
    widths, width = [], 1
    while width < size:
        widths.append(width)
        width *= 3
    return widths


def rotary_tables(total_blocks):
    half = HEAD // 2
    inverse = 10000.0 ** (-np.arange(half, dtype=np.float64) / half)
    sign = np.concatenate([-np.ones(half), np.ones(half)])

    def table(positions):
        angles = positions[:, None] * np.concatenate([inverse, inverse])[None, :]
        return np.cos(angles).astype(np.float32), (np.sin(angles) * sign).astype(np.float32)

    return table(np.arange(BLK, dtype=np.float64)) + table(
        np.arange(total_blocks, dtype=np.float64) * BLK
    )


def kernel(
    n_sp,
    chunks,
    acts_hbm,
    gain_hbm,
    wco_hbm,
    wci_hbm,
    wcv_hbm,
    taps_hbm,
    wq_hbm,
    wk_hbm,
    wv_hbm,
    wg_hbm,
    decay_hbm,
    woc_hbm,
    wor_hbm,
    cos_in_hbm,
    sin_in_hbm,
    cos_off_hbm,
    sin_off_hbm,
    own_out,
    recv_b,
    gain_ref,
    taps_ref,
    decay_ref,
    cos_in_ref,
    sin_in_ref,
    cos_off_ref,
    sin_off_ref,
    x_ref,
    w_ref,
    wo_ref,
    k_ref,
    v_ref,
    q_ref,
    g_ref,
    co_ref,
    ext_ref,
    inner_ref,
    mix_ref,
    st_ref,
    cs_ref,
    sn_ref,
    ld_ref,
    run_ref,
    es_ref,
    el_ref,
    send_s,
    send_l,
    recv_s,
    recv_l,
    send_a,
    recv_a,
    own_ref,
    send_b,
    small_sem,
    out_sem,
    x_sem,
    w_sem,
    scan_send_sem,
    scan_recv_sem,
    rim_sem,
    a_sem,
    b_sem,
):
    sp = lax.axis_index("sp")
    tp = lax.axis_index("tp")
    rows, width = x_ref.shape
    heads = decay_ref.shape[0]
    ch = co_ref.shape[1]
    rc = heads * HEAD
    blocks = rows // BLK
    proj = 256 if rows % 256 == 0 else BLK
    tiles = rows // proj
    widths = windows_of(n_sp)
    distances = [d for w in widths for d in (w, 2 * w) if d < n_sp]
    sibling, across = tp ^ 1, tp ^ 2

    x_copies = [
        pltpu.make_async_copy(
            acts_hbm.at[pl.ds(i * proj, proj)], x_ref.at[pl.ds(i * proj, proj)], x_sem.at[i]
        )
        for i in range(tiles)
    ]
    bounds, w_copies = {}, {}
    start = 0
    for index, (name, ref) in enumerate(
        (
            ("k", wk_hbm),
            ("v", wv_hbm),
            ("q", wq_hbm),
            ("g", wg_hbm),
            ("ci", wci_hbm),
            ("cv", wcv_hbm),
            ("co", wco_hbm),
        )
    ):
        size = ref.shape[1]
        bounds[name] = (start, start + size)
        w_copies[name] = pltpu.make_async_copy(
            ref, w_ref.at[:, pl.ds(start, size)], w_sem.at[index]
        )
        start += size
    w_copies["oc"] = pltpu.make_async_copy(woc_hbm, wo_ref.at[pl.ds(0, ch)], w_sem.at[7])
    w_copies["or"] = pltpu.make_async_copy(wor_hbm, wo_ref.at[pl.ds(ch, rc)], w_sem.at[8])
    small = [
        pltpu.make_async_copy(src, dst, small_sem.at[index])
        for index, (src, dst) in enumerate(
            (
                (decay_hbm, decay_ref),
                (gain_hbm, gain_ref),
                (cos_off_hbm, cos_off_ref),
                (sin_off_hbm, sin_off_ref),
                (cos_in_hbm, cos_in_ref),
                (sin_in_hbm, sin_in_ref),
                (taps_hbm, taps_ref),
            )
        )
    ]
    for copy in small[:2] + x_copies[:1]:
        copy.start()
    w_copies["k"].start()
    w_copies["v"].start()
    for copy in x_copies[1:] + small[2:]:
        copy.start()
    for name in ("q", "g", "ci", "cv", "co", "oc", "or"):
        w_copies[name].start()

    barrier = pltpu.get_barrier_semaphore()
    expected = jnp.int32(2)
    for peer in (sibling, across):
        pl.semaphore_signal(barrier, inc=1, device_id=(sp, peer), device_id_type=MESH)
    for d in distances:
        @pl.when(sp + d < n_sp)
        def _(d=d):
            pl.semaphore_signal(barrier, inc=1, device_id=(sp + d, tp), device_id_type=MESH)

        @pl.when(sp >= d)
        def _(d=d):
            pl.semaphore_signal(barrier, inc=1, device_id=(sp - d, tp), device_id_type=MESH)

        expected = (
            expected
            + jnp.where(sp + d < n_sp, jnp.int32(1), jnp.int32(0))
            + jnp.where(sp >= d, jnp.int32(1), jnp.int32(0))
        )

    small[0].wait()
    ld_ref[...] = jnp.zeros_like(ld_ref)
    for h in range(heads):
        for b in range(blocks):
            j = h * blocks + b
            ld_ref[j : j + 1, :] = decay_ref[h : h + 1, b * BLK : (b + 1) * BLK]
    ld = ld_ref[...]
    row_i = lax.broadcasted_iota(jnp.int32, (BLK, BLK), 0)
    col_i = lax.broadcasted_iota(jnp.int32, (BLK, BLK), 1)
    causal = row_i >= col_i
    upper = jnp.where(row_i <= col_i, 1.0, 0.0).astype(F32)
    lower = jnp.where(row_i >= col_i, 1.0, 0.0).astype(F32)
    after = jnp.where(row_i < col_i, 1.0, 0.0).astype(F32)
    ones = jnp.ones((BLK, BLK), F32)
    nt = (((1,), (1,)), ((), ()))
    level_row = jnp.dot(ld, upper, precision=HI, preferred_element_type=F32)
    total_row = jnp.dot(ld, ones, precision=HI, preferred_element_type=F32)
    level_col = lax.dot_general(lower, ld, nt, precision=HI, preferred_element_type=F32)
    rest_col = lax.dot_general(after, ld, nt, precision=HI, preferred_element_type=F32)
    key_scale = jnp.exp(rest_col)
    query_scale = jnp.exp(level_col)

    small[1].wait()
    gain = gain_ref[...].astype(F32)[None, :]

    def norm_tile(i):
        at = slice(i * proj, (i + 1) * proj)
        x = x_ref[at, :].astype(F32)
        mean_sq = jnp.mean(x * x, axis=-1, keepdims=True)
        x_ref[at, :] = (x * lax.rsqrt(mean_sq + EPS) * gain).astype(BF16)

    x_copies[0].wait()
    norm_tile(0)

    for copy in small[2:]:
        copy.wait()
    for b in range(blocks):
        c_off = cos_off_ref[pl.ds(sp * blocks + b, 1), :]
        s_off = sin_off_ref[pl.ds(sp * blocks + b, 1), :]
        c_in, s_in = cos_in_ref[...], sin_in_ref[...]
        cs_ref[pl.ds(b * BLK, BLK), :] = c_off * c_in - s_off * s_in
        sn_ref[pl.ds(b * BLK, BLK), :] = s_off * c_in + c_off * s_in

    def project(at, first, last):
        lo, hi = bounds[first][0], bounds[last][1]
        return jnp.dot(x_ref[at, :], w_ref[:, lo:hi], preferred_element_type=F32).astype(BF16)

    def rotate(part, at):
        cosine, sine = cs_ref[at, :], sn_ref[at, :]
        turned = []
        for h in range(heads):
            wide = part[:, h * HEAD : (h + 1) * HEAD].astype(F32)
            turned.append((wide * cosine + pltpu.roll(wide, HEAD // 2, 1) * sine).astype(BF16))
        return turned

    def tile_at(i):
        return pl.ds(pl.multiple_of(i * proj, proj), proj)

    w_copies["k"].wait()
    w_copies["v"].wait()
    for copy in x_copies[1:]:
        copy.wait()
    for i in range(tiles):
        at = slice(i * proj, (i + 1) * proj)
        both = project(at, "k", "v")
        if i + 1 < tiles:
            norm_tile(i + 1)
        v_ref[at, :] = both[:, rc:]
        for h, turned in enumerate(rotate(both[:, :rc], at)):
            k_ref[at, h * HEAD : (h + 1) * HEAD] = turned

    device_total = []
    starts = []
    for h in range(heads):
        running = jnp.zeros((HEAD, HEAD), F32)
        total = jnp.zeros((1, HEAD), F32)
        cols = slice(h * HEAD, (h + 1) * HEAD)
        for b in range(blocks):
            j = h * blocks + b
            st_ref[j] = running
            starts.append(total)
            at = slice(b * BLK, (b + 1) * BLK)
            k_dec = (k_ref[at, cols].astype(F32) * key_scale[:, j : j + 1]).astype(BF16)
            contrib = lax.dot_general(
                k_dec, v_ref[at, cols], (((0,), (0,)), ((), ())), preferred_element_type=F32
            )
            running = running * jnp.exp(total_row[j : j + 1, :]) + contrib
            total = total + total_row[j : j + 1, :]
        run_ref[cols, :] = running
        device_total.append(total)

    pl.semaphore_wait(barrier, expected)

    es_ref[...] = jnp.zeros_like(es_ref)
    el_ref[...] = jnp.zeros_like(el_ref)
    send_l[...] = jnp.zeros_like(send_l)

    def scan_copies(r, j, d):
        to = (sp + d, tp)
        return (
            pltpu.make_async_remote_copy(
                src_ref=send_s.at[r],
                dst_ref=recv_s.at[r, j],
                send_sem=scan_send_sem.at[r, j, 0],
                recv_sem=scan_recv_sem.at[r, j, 0],
                device_id=to,
                device_id_type=MESH,
            ),
            pltpu.make_async_remote_copy(
                src_ref=send_l.at[r],
                dst_ref=recv_l.at[r, j],
                send_sem=scan_send_sem.at[r, j, 1],
                recv_sem=scan_recv_sem.at[r, j, 1],
                device_id=to,
                device_id_type=MESH,
            ),
        )

    def scan_send(r):
        for h in range(heads):
            cols = slice(h * HEAD, (h + 1) * HEAD)
            state = run_ref[cols, :]
            if r > 0:
                state = state + jnp.exp(device_total[h]) * es_ref[cols, :]
            send_s[r, cols, :] = state.astype(BF16)
            send_l[r, h : h + 1, :] = device_total[h] + el_ref[h : h + 1, :]
        for j in (1, 0):
            d = (j + 1) * widths[r]
            if d < n_sp:
                @pl.when(sp + d < n_sp)
                def _(j=j, d=d):
                    for copy in scan_copies(r, j, d):
                        copy.start()

    def scan_receive(r):
        for j in range(2):
            d = (j + 1) * widths[r]
            if d < n_sp:
                @pl.when(sp >= d)
                def _(j=j, d=d):
                    for copy in scan_copies(r, j, d):
                        copy.wait_recv()
                    for h in range(heads):
                        cols = slice(h * HEAD, (h + 1) * HEAD)
                        es_ref[cols, :] += jnp.exp(el_ref[h : h + 1, :]) * recv_s[
                            r, j, cols, :
                        ].astype(F32)
                    el_ref[...] += recv_l[r, j]

    scan_send(0)

    w_copies["q"].wait()
    w_copies["g"].wait()

    def qg_tile(i, carry):
        at = tile_at(i)
        both = project(at, "q", "g")
        g_ref[at, :] = both[:, rc:]
        for h, turned in enumerate(rotate(both[:, :rc], at)):
            q_ref[at, h * HEAD : (h + 1) * HEAD] = turned
        return carry

    lax.fori_loop(0, rows // proj, qg_tile, 0)

    for r in range(1, len(widths)):
        scan_receive(r - 1)
        scan_send(r)

    for name in ("ci", "cv", "co"):
        w_copies[name].wait()

    def conv_tile(i, carry):
        at = tile_at(i)
        three = project(at, "ci", "co")
        product = (three[:, :ch].astype(F32) * three[:, ch : 2 * ch].astype(F32)).astype(BF16)
        ext_ref[pl.ds(pl.multiple_of(i * proj + 8, 8), proj), :] = product.astype(F32)
        co_ref[at, :] = three[:, 2 * ch :]
        return carry

    lax.fori_loop(0, rows // proj, conv_tile, 0)

    rim = pltpu.make_async_remote_copy(
        src_ref=ext_ref.at[pl.ds(rows, 8)],
        dst_ref=ext_ref.at[pl.ds(0, 8)],
        send_sem=rim_sem.at[0],
        recv_sem=rim_sem.at[1],
        device_id=(sp + 1, tp),
        device_id_type=MESH,
    )

    @pl.when(sp == 0)
    def _():
        ext_ref[pl.ds(0, 8), :] = jnp.zeros((8, ch), F32)

    @pl.when(sp + 1 < n_sp)
    def _():
        rim.start()

    for h in range(heads):
        cols = slice(h * HEAD, (h + 1) * HEAD)
        for b in range(blocks):
            j = h * blocks + b
            at = slice(b * BLK, (b + 1) * BLK)
            scores = lax.dot_general(q_ref[at, cols], k_ref[at, cols], nt, preferred_element_type=F32)
            diff = level_col[:, j : j + 1] - level_row[j : j + 1, :]
            weights = (scores * jnp.exp(jnp.where(causal, diff, -1e30))).astype(BF16)
            inner_ref[at, cols] = jnp.dot(weights, v_ref[at, cols], preferred_element_type=F32)

    @pl.when(sp >= 1)
    def _():
        rim.wait_recv()

    taps = taps_ref[...].astype(F32)
    for b in range(blocks):
        at = slice(b * BLK, (b + 1) * BLK)
        base = b * BLK + 8 - (CONV_W - 1)
        filtered = taps[0:1, :] * ext_ref[base : base + BLK, :]
        for t in range(1, CONV_W):
            filtered = filtered + taps[t : t + 1, :] * ext_ref[base + t : base + t + BLK, :]
        mix_ref[at, 0:ch] = (co_ref[at, :].astype(F32) * filtered).astype(BF16)

    scan_receive(len(widths) - 1)

    for b in range(blocks):
        at = slice(b * BLK, (b + 1) * BLK)
        for h in range(heads):
            cols = slice(h * HEAD, (h + 1) * HEAD)
            j = h * blocks + b
            state = (st_ref[j] + jnp.exp(starts[j]) * es_ref[cols, :]).astype(BF16)
            q_dec = (q_ref[at, cols].astype(F32) * query_scale[:, j : j + 1]).astype(BF16)
            retained = inner_ref[at, cols] + jnp.dot(q_dec, state, preferred_element_type=F32)
            mean_sq = jnp.mean(retained * retained, axis=-1, keepdims=True)
            gate = g_ref[at, cols].astype(F32)
            gate = gate / (1.0 + jnp.exp(-gate))
            mix_ref[at, ch + h * HEAD : ch + (h + 1) * HEAD] = (
                retained * lax.rsqrt(mean_sq + EPS) * gate
            ).astype(BF16)

    w_copies["oc"].wait()
    w_copies["or"].wait()
    part = own_out.shape[0]
    wide = width // chunks

    def partial(block, c):
        at = pl.ds(pl.multiple_of(block * part, 16), part)
        return jnp.dot(
            mix_ref[at, :], wo_ref[:, c * wide : (c + 1) * wide], preferred_element_type=F32
        )

    def to_sibling(p, c):
        return pltpu.make_async_remote_copy(
            src_ref=send_a.at[p, c],
            dst_ref=recv_a.at[p, c],
            send_sem=a_sem.at[0, p, c],
            recv_sem=a_sem.at[1, p, c],
            device_id=(sp, sibling),
            device_id_type=MESH,
        )

    def to_across(c):
        return pltpu.make_async_remote_copy(
            src_ref=send_b.at[c],
            dst_ref=recv_b.at[:, pl.ds(c * wide, wide)],
            send_sem=b_sem.at[0, c],
            recv_sem=b_sem.at[1, c],
            device_id=(sp, across),
            device_id_type=MESH,
        )

    def send_sibling(p, c):
        send_a[p, c] = partial(tp ^ (3 if p == 0 else 1), c).astype(BF16)
        to_sibling(p, c).start()

    def send_across(c):
        own = partial(across, c)
        to_sibling(0, c).wait_recv()
        send_b[c] = (own + recv_a[0, c].astype(F32)).astype(BF16)
        to_across(c).start()

    send_sibling(0, 0)
    for c in range(chunks):
        if c + 1 < chunks:
            send_sibling(0, c + 1)
        send_across(c)
    for c in range(chunks):
        send_sibling(1, c)
    outs = [
        pltpu.make_async_copy(
            own_ref.at[c], own_out.at[:, pl.ds(c * wide, wide)], out_sem.at[c]
        )
        for c in range(chunks)
    ]
    for c in range(chunks):
        own = partial(tp, c)
        to_sibling(1, c).wait_recv()
        own_ref[c] = (own + recv_a[1, c].astype(F32)).astype(BF16)
        outs[c].start()

    for r in range(len(widths)):
        for j in range(2):
            d = (j + 1) * widths[r]
            if d < n_sp:
                @pl.when(sp + d < n_sp)
                def _(r=r, j=j, d=d):
                    for copy in scan_copies(r, j, d):
                        copy.wait_send()

    @pl.when(sp + 1 < n_sp)
    def _():
        rim.wait_send()

    for c in range(chunks):
        to_sibling(0, c).wait_send()
        to_sibling(1, c).wait_send()
        outs[c].wait()
        to_across(c).wait()


def local(
    n_sp,
    n_tp,
    activations,
    norm_gain,
    w_conv_outer,
    w_conv_inner,
    w_conv_value,
    conv_taps,
    w_query,
    w_key,
    w_value,
    w_gate,
    log_decay,
    w_out_conv,
    w_out_ret,
):
    rows, width = activations.shape
    heads = log_decay.shape[0]
    blocks = rows // BLK
    ch = w_conv_outer.shape[1]
    rc = heads * HEAD
    part = rows // n_tp
    chunks = 8
    wide = width // chunks
    rounds = len(windows_of(n_sp))
    pad = -(-heads * blocks // 8) * 8
    tables = [jnp.asarray(t) for t in rotary_tables(n_sp * blocks)]
    hbm = pl.BlockSpec(memory_space=pl.ANY)
    dma = pltpu.SemaphoreType.DMA
    own, received = pl.pallas_call(
        functools.partial(kernel, n_sp, chunks),
        out_shape=[jax.ShapeDtypeStruct((part, width), BF16)] * 2,
        in_specs=[hbm] * 17,
        out_specs=[hbm] * 2,
        scratch_shapes=[
            pltpu.VMEM(norm_gain.shape, BF16),
            pltpu.VMEM(conv_taps.shape, BF16),
            pltpu.VMEM(log_decay.shape, F32),
            pltpu.VMEM((BLK, HEAD), F32),
            pltpu.VMEM((BLK, HEAD), F32),
            pltpu.VMEM((n_sp * blocks, HEAD), F32),
            pltpu.VMEM((n_sp * blocks, HEAD), F32),
            pltpu.VMEM((rows, width), BF16),
            pltpu.VMEM((width, 3 * ch + 4 * rc), BF16),
            pltpu.VMEM((ch + rc, width), BF16),
            pltpu.VMEM((rows, rc), BF16),
            pltpu.VMEM((rows, rc), BF16),
            pltpu.VMEM((rows, rc), BF16),
            pltpu.VMEM((rows, rc), BF16),
            pltpu.VMEM((rows, ch), BF16),
            pltpu.VMEM((rows + 8, ch), F32),
            pltpu.VMEM((rows, rc), F32),
            pltpu.VMEM((rows, ch + rc), BF16),
            pltpu.VMEM((heads * blocks, HEAD, HEAD), F32),
            pltpu.VMEM((rows, HEAD), F32),
            pltpu.VMEM((rows, HEAD), F32),
            pltpu.VMEM((pad, BLK), F32),
            pltpu.VMEM((rc, HEAD), F32),
            pltpu.VMEM((rc, HEAD), F32),
            pltpu.VMEM((8, HEAD), F32),
            pltpu.VMEM((rounds, rc, HEAD), BF16),
            pltpu.VMEM((rounds, 8, HEAD), F32),
            pltpu.VMEM((rounds, 2, rc, HEAD), BF16),
            pltpu.VMEM((rounds, 2, 8, HEAD), F32),
            pltpu.VMEM((2, chunks, part, wide), BF16),
            pltpu.VMEM((2, chunks, part, wide), BF16),
            pltpu.VMEM((chunks, part, wide), BF16),
            pltpu.VMEM((chunks, part, wide), BF16),
            dma((7,)),
            dma((chunks,)),
            dma((blocks,)),
            dma((9,)),
            dma((rounds, 2, 2)),
            dma((rounds, 2, 2)),
            dma((2,)),
            dma((2, 2, chunks)),
            dma((2, chunks)),
        ],
        compiler_params=pltpu.CompilerParams(
            collective_id=0, has_side_effects=True, vmem_limit_bytes=60 * 1024 * 1024
        ),
    )(
        activations,
        norm_gain,
        w_conv_outer,
        w_conv_inner,
        w_conv_value,
        conv_taps,
        w_query,
        w_key,
        w_value,
        w_gate,
        log_decay,
        w_out_conv,
        w_out_ret,
        *tables,
    )
    return (own.astype(F32) + received.astype(F32)).astype(BF16)


def solution(mesh):
    return jax.shard_map(
        functools.partial(local, mesh.shape["sp"], mesh.shape["tp"]),
        mesh=mesh,
        in_specs=(
            P("sp", None),
            P(),
            P(None, "tp"),
            P(None, "tp"),
            P(None, "tp"),
            P(None, "tp"),
            P(None, "tp"),
            P(None, "tp"),
            P(None, "tp"),
            P(None, "tp"),
            P("tp", "sp"),
            P("tp", None),
            P("tp", None),
        ),
        out_specs=P(("sp", "tp"), None),
        check_vma=False,
    )
```
